32 devices in a mesh: dp: 4 (over y, x), kv: 4 (over z), tp: 2 (over core).
Axes of the slice: x: 2, y: 2, z: 4, core: 2. Of those that a mesh axis runs over, the one named last changes fastest.
Arguments:
- tokens: bfloat16 [4, 2048, 1024], P('dp', ('kv', 'tp')), may hold values from -6 to 6
- w_query: bfloat16 [1024, 1024], P(None, 'tp'), may hold values from -0.1875 to 0.1875
- w_key: bfloat16 [1024, 256], P(None, 'tp'), may hold values from -0.1875 to 0.1875
- w_value: bfloat16 [1024, 256], P(None, 'tp'), may hold values from -0.1875 to 0.1875
- w_out: bfloat16 [1024, 1024], P('tp'), may hold values from -0.1875 to 0.1875
- chosen: int32 [4, 32, 15], P('dp', 'kv'), may hold values from -1 to 30, as said below
Outputs:
- normed: bfloat16 [4, 2048, 1024], P('dp', ('kv', 'tp'))
- logsums: float32 [4, 2048, 16], P('dp', 'kv', 'tp')
The draws below stay inside these ranges and needn't reach their ends.
Inputs may be any that keep to these rules, and one draw needn't show every extreme that they name: Each entry of chosen[s, c] is -1 or a block below c; entries of a row that are not -1 differ. Within a sequence, the 15 times 8 entries of the query blocks of one aligned run of 8 blocks name at most 4 different blocks inside any one aligned run, and some run pair reaches exactly 4.
All inputs are finite; a program needn't handle non-finite values.
Results may differ from the reference program's by a relative error of at most 0.0085.
Values may be sent and summed in bfloat16 or wider, within the bound.
A program may use at most 64 MiB of HBM per device.

```python
import jax
import jax.numpy as jnp
from jax import lax

D = 1024
HEADS = 16
KV_HEADS = 4
HEAD_DIM = 64
BLK = 64
PICK = 15
CAP = 4
TOK_DEV = 512
SEQS = 4
SEQ = 2048
NBLK = 32


def draw_chosen(key, part):
    local_blocks = TOK_DEV // BLK
    owner_count = NBLK // local_blocks
    key_pool = jax.random.fold_in(key, 11)
    key_popular = jax.random.fold_in(key, 23)
    key_noise = jax.random.fold_in(key, 37)
    pool_scores = jax.random.randint(key_pool, (SEQS, owner_count, owner_count, local_blocks), 0, 4096) * local_blocks
    pool_scores = pool_scores + jnp.arange(local_blocks, dtype=jnp.int32)
    ranking = jnp.argsort(jnp.argsort(pool_scores, axis=-1, stable=True), axis=-1, stable=True)
    member = (ranking < CAP).reshape(SEQS, owner_count, NBLK)
    blocks = jnp.arange(NBLK, dtype=jnp.int32)
    owners = blocks // local_blocks
    earlier_owner = owners[None, :] <= jnp.arange(owner_count, dtype=jnp.int32)[:, None]
    member = member & earlier_owner[None]
    candidate = member[:, owners, :] & (blocks[None, :] < blocks[:, None])[None]
    last_block = blocks % local_blocks == local_blocks - 1
    forced = last_block[:, None] & (owners[None, :] == owners[:, None] - 1)
    popularity = jax.random.randint(key_popular, (SEQS, owner_count), 0, 8)
    noise = jax.random.randint(key_noise, (SEQS, NBLK, NBLK), 0, 2048)
    score = candidate.astype(jnp.int32) * 2 ** 27
    score = score + (forced[None] & candidate).astype(jnp.int32) * 2 ** 26
    score = score + popularity[:, None, :][:, :, owners] * 2 ** 22
    score = score + noise * NBLK + blocks[None, None, :]
    ordered, picked = lax.top_k(score, PICK)
    taken = jnp.take_along_axis(candidate, picked, axis=-1)
    return jnp.where(taken, picked, -1).astype(jnp.int32)


def level_of(own_key, extent, pieces, low, largest):
    gain = 1.0
    for position, parts in pieces:
        steps = jax.random.uniform(jax.random.fold_in(jax.random.fold_in(own_key, 6), position), (parts,), jnp.float32, low / len(pieces), largest / len(pieces))
        gain = gain * jnp.repeat(jnp.exp(steps), extent[position] // parts).reshape((-1,) + (1,) * (len(extent) - 1 - position))
    return gain


def normal_values(key, shape, width, reach, pieces=(), held_as=jnp.bfloat16):
    drawn = jax.random.normal(key, shape, jnp.float32) * width
    if len(pieces) > 0:
        drawn = level_of(key, shape, pieces, -0.22, 0.18) * drawn
    return jnp.clip(drawn, min=-reach, max=reach).astype(held_as)


def setup_inputs(seed: int = 0) -> dict:
    seeds = jax.random.split(jax.random.key(seed), 7)
    tokens = normal_values(seeds[0], (SEQS, SEQ, D), 1.0, 6.0, ((0, 4), (1, 8)))
    w_query = normal_values(seeds[1], (D, HEADS * HEAD_DIM), D ** -0.5, 0.1875, ((1, 2),))
    w_key = normal_values(seeds[2], (D, KV_HEADS * HEAD_DIM), D ** -0.5, 0.1875, ((1, 2),))
    w_value = normal_values(seeds[3], (D, KV_HEADS * HEAD_DIM), D ** -0.5, 0.1875, ((1, 2),))
    w_out = normal_values(seeds[4], (HEADS * HEAD_DIM, D), (HEADS * HEAD_DIM) ** -0.5, 0.1875, ((0, 2),))
    chosen = draw_chosen(jax.random.fold_in(seeds[6], 71), 0)
    return {"tokens": tokens, "w_query": w_query, "w_key": w_key, "w_value": w_value, "w_out": w_out, "chosen": chosen}


THETA_BASE = 10000.0
NEGATIVE = -1e+30
EPSILON = 1e-06

def rotate(values_in, positions):
    half_width = values_in.shape[-1] // 2
    inverse = THETA_BASE ** (-jnp.arange(half_width, dtype=jnp.float32) / half_width)
    angles = positions.astype(jnp.float32)[:, None] * inverse[None, :]
    cosine_table = jnp.cos(angles)[:, None, :]
    sine_table = jnp.sin(angles)[:, None, :]
    as_float = values_in.astype(jnp.float32)
    first_half = as_float[..., :half_width]
    second_half = as_float[..., half_width:]
    joined = jnp.concatenate([first_half * cosine_table - second_half * sine_table, second_half * cosine_table + first_half * sine_table], axis=-1)
    return joined.astype(jnp.bfloat16)

def attend(queries, key_rows, value_rows, usable):
    scores = jnp.einsum('qkgd,nkd->kgqn', queries.astype(jnp.float32), key_rows.astype(jnp.float32))
    scores = scores * HEAD_DIM ** (-0.5)
    scores = jnp.where(usable[None, None], scores, NEGATIVE)
    maximum = lax.optimization_barrier(jnp.max(scores, axis=-1, keepdims=True))
    exponent = jnp.exp(scores - maximum)
    denominator = lax.optimization_barrier(jnp.sum(exponent, axis=-1, keepdims=True))
    logsum = (maximum + jnp.log(denominator))[..., 0]
    weights = (exponent / denominator).astype(jnp.bfloat16)
    combined = jnp.einsum('kgqn,nkd->qkgd', weights.astype(jnp.float32), value_rows.astype(jnp.float32))
    block_rows = queries.shape[0]
    return (combined.astype(jnp.bfloat16).reshape(block_rows, -1), jnp.transpose(logsum, (2, 0, 1)).reshape(block_rows, -1))

def block_mask(usable_picks):
    picked_keys = jnp.repeat(usable_picks, BLK)
    earlier = jnp.broadcast_to(picked_keys[None, :], (BLK, PICK * BLK))
    query_pos = jnp.arange(BLK, dtype=jnp.int32)
    causal = query_pos[None, :] <= query_pos[:, None]
    return jnp.concatenate([earlier, causal], axis=1)

def reference(tokens, w_query, w_key, w_value, w_out, chosen):
    group_size = HEADS // KV_HEADS
    positions = jnp.arange(SEQ, dtype=jnp.int32)

    def one_sequence(element):
        rows_in, chosen_rows = element
        queries = jnp.dot(rows_in, w_query, preferred_element_type=jnp.float32).astype(jnp.bfloat16)
        key_rows = jnp.dot(rows_in, w_key, preferred_element_type=jnp.float32).astype(jnp.bfloat16)
        value_rows = jnp.dot(rows_in, w_value, preferred_element_type=jnp.float32).astype(jnp.bfloat16)
        queries = rotate(queries.reshape(SEQ, HEADS, HEAD_DIM), positions)
        key_rows = rotate(key_rows.reshape(SEQ, KV_HEADS, HEAD_DIM), positions)
        value_rows = value_rows.reshape(SEQ, KV_HEADS, HEAD_DIM)
        query_blocks = queries.reshape(NBLK, BLK, KV_HEADS, group_size, HEAD_DIM)
        key_blocks = key_rows.reshape(NBLK, BLK, KV_HEADS, HEAD_DIM)
        value_blocks = value_rows.reshape(NBLK, BLK, KV_HEADS, HEAD_DIM)

        def one_block(item):
            block_index, block_picks = item
            usable_picks = block_picks >= 0
            safe_index = jnp.maximum(block_picks, 0).astype(jnp.int32)
            gathered_keys = jnp.concatenate([key_blocks[safe_index].reshape(PICK * BLK, KV_HEADS, HEAD_DIM), key_blocks[block_index]], axis=0)
            gathered_values = jnp.concatenate([value_blocks[safe_index].reshape(PICK * BLK, KV_HEADS, HEAD_DIM), value_blocks[block_index]], axis=0)
            return attend(query_blocks[block_index], gathered_keys, gathered_values, block_mask(usable_picks))
        outputs, block_logs = lax.map(one_block, (jnp.arange(NBLK, dtype=jnp.int32), chosen_rows))
        attended = outputs.reshape(SEQ, HEADS * HEAD_DIM)
        projected = jnp.dot(attended, w_out, preferred_element_type=jnp.float32)
        scale_rows = lax.rsqrt(lax.optimization_barrier(jnp.mean(projected * projected, axis=-1, keepdims=True)) + EPSILON)
        return ((projected * scale_rows).astype(jnp.bfloat16), block_logs.reshape(SEQ, HEADS))
    normed, logsums = lax.map(one_sequence, (tokens, chosen))
    return (normed, logsums)
```

```python
import functools
import math

import jax
import jax.numpy as jnp
from jax import lax
from jax.experimental import pallas as pl
from jax.experimental.pallas import tpu as pltpu
from jax.sharding import PartitionSpec as P

HEAD_DIM = 64
BLK = 64
CAP = 4
THETA_BASE = 10000.0
NEGATIVE = -1e30
EPSILON = 1e-06
MESH = pl.DeviceIdType.MESH
F32 = jnp.float32
BF16 = jnp.bfloat16
NT = (((1,), (1,)), ((), ()))
NN = (((1,), (0,)), ((), ()))


def mm(a, b, dims=NN):
    return lax.dot_general(a, b, dims, preferred_element_type=F32)


def iota(shape, dim):
    return lax.broadcasted_iota(jnp.int32, shape, dim)


def kernel(
    n,
    chosen_ref,
    tokens_hbm,
    wq_hbm,
    wk_hbm,
    wv_hbm,
    wo_hbm,
    normed_ref,
    logs_ref,
    tok,
    wq,
    wkv,
    wo,
    cos_t,
    sin_t,
    pick,
    bias,
    keys,
    vals_t,
    sel_k,
    sel_v,
    got_k,
    got_v,
    qaug,
    m_s,
    l_s,
    acc,
    att,
    send_p,
    recv_p,
    load_sem,
    tok_sem,
    pick_send,
    pick_recv,
    k_send,
    k_recv,
    v_send,
    v_recv,
    p_send,
    p_recv,
):
    me = lax.axis_index("kv")
    half = lax.axis_index("tp")
    other = 1 - half
    rows = tok.shape[0]
    mine = rows // 2
    blocks = rows // BLK
    groups = wq.shape[1] // (2 * HEAD_DIM)
    slot_keys = CAP * BLK
    lanes_all = groups * BLK

    own_rows = pl.ds(pl.multiple_of(half * mine, mine), mine)
    ld_tok = pltpu.make_async_copy(tokens_hbm.at[0], tok.at[own_rows], load_sem.at[0])
    ld_k = pltpu.make_async_copy(wk_hbm, wkv.at[:, 0:128], load_sem.at[1])
    ld_v = pltpu.make_async_copy(wv_hbm, wkv.at[:, 128:256], load_sem.at[2])
    ld_q = pltpu.make_async_copy(wq_hbm, wq, load_sem.at[3])
    ld_tok.start()
    ld_k.start()
    ld_v.start()
    ld_q.start()
    ld_o = []
    for h in range(2):
        for g in range(groups):
            source = (h * groups + g) * HEAD_DIM
            target = (g * 2 + h) * HEAD_DIM
            ld_o.append(
                pltpu.make_async_copy(
                    wo_hbm.at[source : source + HEAD_DIM],
                    wo.at[target : target + HEAD_DIM],
                    load_sem.at[4 + h * groups + g],
                )
            )
    for copy in ld_o:
        copy.start()

    barrier = pltpu.get_barrier_semaphore()
    pl.semaphore_signal(barrier, inc=1, device_id={"tp": other}, device_id_type=MESH)
    for d in range(1, n):
        pl.semaphore_signal(
            barrier, inc=1, device_id={"kv": lax.rem(me + d, n)}, device_id_type=MESH
        )

    npad = pick.shape[2]
    chosen = chosen_ref[0]
    block_ids = iota((blocks, npad), 1)
    picked = jnp.zeros((blocks, npad), F32)
    for k in range(chosen.shape[1]):
        picked = picked + (chosen[:, k : k + 1] == block_ids).astype(F32)
    pick[0] = picked

    pl.semaphore_wait(barrier, n)
    ld_tok.wait()
    tok_copy = pltpu.make_async_remote_copy(
        src_ref=tok.at[own_rows],
        dst_ref=tok.at[own_rows],
        send_sem=tok_sem.at[0],
        recv_sem=tok_sem.at[1],
        device_id={"tp": other},
        device_id_type=MESH,
    )
    tok_copy.start()

    def pick_copy(d, target):
        return pltpu.make_async_remote_copy(
            src_ref=pick.at[0],
            dst_ref=pick.at[d],
            send_sem=pick_send.at[d],
            recv_sem=pick_recv.at[d],
            device_id={"kv": target},
            device_id_type=MESH,
        )

    @pl.loop(1, me + 1)
    def _(d):
        pick_copy(d, me - d).start()

    lane = iota((1, 128), 1)
    inverse = jnp.exp((lane % 32).astype(F32) * (-math.log(THETA_BASE) / 32))
    sign = jnp.where(lane % 64 < 32, -1.0, 1.0)
    inner = iota((BLK, 128), 0).astype(F32) * inverse
    cos_in, sin_in = jnp.cos(inner), jnp.sin(inner)
    starts = (me * rows + iota((blocks, 128), 0) * BLK).astype(F32) * inverse
    cos_st, sin_st = jnp.cos(starts), jnp.sin(starts)
    for c in range(blocks):
        part = slice(c * BLK, (c + 1) * BLK)
        cs, sn = cos_st[c : c + 1], sin_st[c : c + 1]
        cos_t[part] = cs * cos_in - sn * sin_in
        sin_t[part] = (sn * cos_in + cs * sin_in) * sign

    slots = bias.shape[0]
    nslots = slots // slot_keys * CAP

    def slot_table(marks):
        needed = (jnp.max(marks, axis=0, keepdims=True) > 0).astype(F32)
        b_in, b_out = iota((npad, npad), 0), iota((npad, npad), 1)
        before = ((b_in // blocks == b_out // blocks) & (b_in < b_out)).astype(BF16)
        rank = mm(jnp.broadcast_to(needed, (8, npad)).astype(BF16), before)[0:1]
        rank = rank.astype(jnp.int32)
        place = iota((1, npad), 1) // blocks * CAP + rank
        fits = (needed > 0) & (rank < CAP)
        return jnp.where((iota((nslots, npad), 0) == place) & fits, 1.0, 0.0).astype(BF16)

    table = slot_table(picked)
    zero_rows = jnp.zeros((HEAD_DIM - blocks, npad), F32)
    twice = jnp.concatenate([picked, zero_rows, picked, zero_rows], axis=0).astype(BF16)
    reads = mm(table, twice, NT)
    lane_n = iota((nslots, 128), 1)
    reads = jnp.where(lane_n % 64 < blocks, (1.0 - reads) * NEGATIVE, 0.0).astype(BF16)
    spread = (iota((slots, nslots), 0) // BLK == iota((slots, nslots), 1)).astype(BF16)
    bias[...] = mm(spread, reads).astype(BF16)

    def rope(x, part):
        turned = jnp.where(
            iota(x.shape, 1) % 64 < 32, pltpu.roll(x, 96, 1), pltpu.roll(x, 32, 1)
        )
        return x * cos_t[part] + turned * sin_t[part]

    ld_k.wait()
    ld_v.wait()

    def project_kv(part):
        out = mm(tok[part], wkv[...]).astype(BF16)
        keys[part] = rope(out[:, 0:128].astype(F32), part).astype(BF16)
        return out[:, 128:256]

    mine_part = pl.ds(pl.multiple_of(half * mine, mine), mine)
    other_part = pl.ds(pl.multiple_of(other * mine, mine), mine)
    v_mine = project_kv(mine_part).astype(F32).T.astype(BF16)
    vals_t[:, mine_part] = v_mine
    tok_copy.wait_recv()
    v_other = project_kv(other_part).astype(F32).T.astype(BF16)
    vals_t[:, other_part] = v_other

    def select(tab, d):
        first = (
            iota((slot_keys, nslots), 1) == me * CAP + iota((slot_keys, nslots), 0) // BLK
        ).astype(BF16)
        last = (iota((npad, rows), 0) == me * blocks + iota((npad, rows), 1) // BLK).astype(BF16)
        chain = mm(mm(first, tab).astype(BF16), last)
        same = iota((slot_keys, rows), 0) % BLK == iota((slot_keys, rows), 1) % BLK
        hot = jnp.where(same, chain, 0.0).astype(BF16)
        sel_k[d] = mm(hot, keys[...]).astype(BF16)
        sel_v[d] = mm(vals_t[...], hot, NT).astype(BF16)

    def key_copy(d, target):
        return pltpu.make_async_remote_copy(
            src_ref=sel_k.at[d],
            dst_ref=got_k.at[d],
            send_sem=k_send.at[d],
            recv_sem=k_recv.at[d],
            device_id={"kv": target},
            device_id_type=MESH,
        )

    def value_copy(d, target):
        return pltpu.make_async_remote_copy(
            src_ref=sel_v.at[d],
            dst_ref=got_v.at[d],
            send_sem=v_send.at[d],
            recv_sem=v_recv.at[d],
            device_id={"kv": target},
            device_id_type=MESH,
        )

    @pl.loop(1, n - me)
    def _(d):
        pick_copy(d, me).wait_recv()
        select(slot_table(pick[d]), d)
        key_copy(d, me + d).start()
        value_copy(d, me + d).start()

    select(table, 0)

    ld_q.wait()

    @pl.loop(0, blocks)
    def _(c):
        part = pl.ds(pl.multiple_of(c * BLK, BLK), BLK)
        q = mm(tok[part], wq[...]).astype(BF16).astype(F32)
        tiles = [
            rope(q[:, t * 128 : (t + 1) * 128], part) * HEAD_DIM**-0.5 for t in range(groups)
        ]
        low = iota((BLK, 128), 1) < 64
        hot = (iota((BLK, 128), 1) % 64 == c).astype(F32)
        for g in range(groups):
            a, b = tiles[g // 2], tiles[groups // 2 + g // 2]
            if g % 2 == 0:
                both = jnp.where(low, a, pltpu.roll(b, 64, 1))
            else:
                both = jnp.where(low, pltpu.roll(a, 64, 1), b)
            place = slice(g * BLK, (g + 1) * BLK)
            qaug[c, 0, place] = jnp.where(low, both, hot).astype(BF16)
            qaug[c, 1, place] = jnp.where(low, hot, both).astype(BF16)

    def widened(k, extra, h):
        low = iota(k.shape, 1) < 64
        return jnp.where(low, k, extra) if h == 0 else jnp.where(low, extra, k)

    own_bias = bias[pl.ds(pl.multiple_of(me * slot_keys, slot_keys), slot_keys)]

    @pl.loop(0, blocks)
    def _(c):
        part = pl.ds(pl.multiple_of(c * BLK, BLK), BLK)
        for h in range(2):
            q = qaug[c, h]
            s = mm(widened(sel_k[0], own_bias, h), q, NT)
            k_own = keys[part]
            s_own = mm(widened(k_own, jnp.zeros_like(k_own), h), q, NT)
            ok = iota((BLK, lanes_all), 0) <= iota((BLK, lanes_all), 1) % BLK
            s_own = jnp.where(ok, s_own, NEGATIVE)
            m = jnp.maximum(
                jnp.max(s, axis=0, keepdims=True), jnp.max(s_own, axis=0, keepdims=True)
            )
            p = jnp.exp(s - m)
            p_own = jnp.exp(s_own - m)
            m_s[c, h] = m
            l_s[c, h] = jnp.sum(p, axis=0, keepdims=True) + jnp.sum(p_own, axis=0, keepdims=True)
            head = slice(h * HEAD_DIM, (h + 1) * HEAD_DIM)
            block_hot = (
                iota((BLK, rows), 1) == c * BLK + iota((BLK, rows), 0)
            ).astype(BF16)
            v_own = mm(vals_t[head], block_hot, NT).astype(BF16)
            acc[c, h] = mm(sel_v[0, head], p.astype(BF16)) + mm(v_own, p_own.astype(BF16))

    @pl.loop(1, me + 1)
    def _(d):
        key_copy(d, me).wait_recv()
        value_copy(d, me).wait_recv()
        owner = me - d
        extra = bias[pl.ds(pl.multiple_of(owner * slot_keys, slot_keys), slot_keys)]
        ks = [widened(got_k[d], extra, h) for h in range(2)]

        @pl.loop(0, blocks)
        def _(c):
            for h in range(2):
                s = mm(ks[h], qaug[c, h], NT)
                m_old = m_s[c, h]
                m = jnp.maximum(m_old, jnp.max(s, axis=0, keepdims=True))
                shrink = jnp.exp(m_old - m)
                p = jnp.exp(s - m)
                m_s[c, h] = m
                l_s[c, h] = l_s[c, h] * shrink + jnp.sum(p, axis=0, keepdims=True)
                head = slice(h * HEAD_DIM, (h + 1) * HEAD_DIM)
                acc[c, h] = acc[c, h] * shrink + mm(got_v[d, head], p.astype(BF16))

    @pl.loop(0, blocks)
    def _(c):
        part = pl.ds(pl.multiple_of(c * BLK, BLK), BLK)
        sums = [l_s[c, h] for h in range(2)]
        both = jnp.concatenate([acc[c, h] / sums[h] for h in range(2)], axis=0).T
        for g in range(groups):
            att[part, g * 128 : (g + 1) * 128] = both[g * BLK : (g + 1) * BLK].astype(BF16)
        logs = [m_s[c, h] + jnp.log(sums[h]) for h in range(2)]
        stacked = jnp.concatenate(
            [logs[h][:, g * BLK : (g + 1) * BLK] for h in range(2) for g in range(groups)],
            axis=0,
        )
        logs_ref[0, part] = stacked.T

    for copy in ld_o:
        copy.wait()
    pieces = send_p.shape[0]
    step = mine // pieces

    def sum_copy(i):
        return pltpu.make_async_remote_copy(
            src_ref=send_p.at[i],
            dst_ref=recv_p.at[i],
            send_sem=p_send.at[i],
            recv_sem=p_recv.at[i],
            device_id={"tp": other},
            device_id_type=MESH,
        )

    for i in range(pieces):
        part = pl.ds(pl.multiple_of(other * mine + i * step, step), step)
        send_p[i] = mm(att[part], wo[...])
        sum_copy(i).start()
    for i in range(pieces):
        part = pl.ds(pl.multiple_of(half * mine + i * step, step), step)
        own = mm(att[part], wo[...])
        sum_copy(i).wait_recv()
        total = own + recv_p[i]
        scale = lax.rsqrt(jnp.mean(total * total, axis=-1, keepdims=True) + EPSILON)
        normed_ref[0, i * step : (i + 1) * step] = (total * scale).astype(BF16)

    tok_copy.wait_send()
    for i in range(pieces):
        sum_copy(i).wait_send()

    @pl.loop(1, me + 1)
    def _(d):
        pick_copy(d, me).wait_send()

    @pl.loop(1, n - me)
    def _(d):
        key_copy(d, me).wait_send()
        value_copy(d, me).wait_send()


def shards(tokens, w_query, w_key, w_value, w_out, chosen):
    n = lax.axis_size("kv")
    mine, width = tokens.shape[1], tokens.shape[2]
    rows = 2 * mine
    blocks = rows // BLK
    heads = w_query.shape[1] // HEAD_DIM
    groups = heads // 2
    npad = -(-n * blocks // 128) * 128
    slot_keys = CAP * BLK
    lanes_all = groups * BLK
    pieces = 2
    dma = pltpu.SemaphoreType.DMA
    vmem = pl.BlockSpec(memory_space=pltpu.VMEM)
    hbm = pl.BlockSpec(memory_space=pl.ANY)
    return pl.pallas_call(
        functools.partial(kernel, n),
        out_shape=(
            jax.ShapeDtypeStruct((1, mine, width), BF16),
            jax.ShapeDtypeStruct((1, rows, heads), F32),
        ),
        in_specs=[vmem, hbm, hbm, hbm, hbm, hbm],
        out_specs=(vmem, vmem),
        scratch_shapes=[
            pltpu.VMEM((rows, width), BF16),
            pltpu.VMEM(w_query.shape, BF16),
            pltpu.VMEM((width, 256), BF16),
            pltpu.VMEM(w_out.shape, BF16),
            pltpu.VMEM((rows, 128), F32),
            pltpu.VMEM((rows, 128), F32),
            pltpu.VMEM((n, blocks, npad), F32),
            pltpu.VMEM((n * slot_keys, 128), BF16),
            pltpu.VMEM((rows, 128), BF16),
            pltpu.VMEM((128, rows), BF16),
            pltpu.VMEM((n, slot_keys, 128), BF16),
            pltpu.VMEM((n, 128, slot_keys), BF16),
            pltpu.VMEM((n, slot_keys, 128), BF16),
            pltpu.VMEM((n, 128, slot_keys), BF16),
            pltpu.VMEM((blocks, 2, lanes_all, 128), BF16),
            pltpu.VMEM((blocks, 2, 1, lanes_all), F32),
            pltpu.VMEM((blocks, 2, 1, lanes_all), F32),
            pltpu.VMEM((blocks, 2, HEAD_DIM, lanes_all), F32),
            pltpu.VMEM((rows, heads * HEAD_DIM), BF16),
            pltpu.VMEM((pieces, mine // pieces, width), F32),
            pltpu.VMEM((pieces, mine // pieces, width), F32),
            dma((4 + heads,)),
            dma((2,)),
            dma((n,)),
            dma((n,)),
            dma((n,)),
            dma((n,)),
            dma((n,)),
            dma((n,)),
            dma((pieces,)),
            dma((pieces,)),
        ],
        compiler_params=pltpu.CompilerParams(
            collective_id=0, has_side_effects=True, vmem_limit_bytes=48 * 1024 * 1024
        ),
    )(chosen, tokens, w_query, w_key, w_value, w_out)


def solution(mesh):
    placed = (
        P("dp", ("kv", "tp"), None),
        P(None, "tp"),
        P(None, "tp"),
        P(None, "tp"),
        P("tp", None),
        P("dp", "kv", None),
    )
    return jax.shard_map(
        shards,
        mesh=mesh,
        in_specs=placed,
        out_specs=(P("dp", ("kv", "tp"), None), P("dp", "kv", "tp")),
        check_vma=False,
    )
```

```python
import functools
import math

import jax
import jax.numpy as jnp
from jax import lax
from jax.experimental import pallas as pl
from jax.experimental.pallas import tpu as pltpu
from jax.sharding import PartitionSpec as P

HEAD_DIM = 64
BLK = 64
CAP = 4
THETA_BASE = 10000.0
NEGATIVE = -1e30
EPSILON = 1e-06
MESH = pl.DeviceIdType.MESH
F32 = jnp.float32
BF16 = jnp.bfloat16
NT = (((1,), (1,)), ((), ()))
NN = (((1,), (0,)), ((), ()))


def mm(a, b, dims=NN):
    return lax.dot_general(a, b, dims, preferred_element_type=F32)


def iota(shape, dim):
    return lax.broadcasted_iota(jnp.int32, shape, dim)


def kernel(
    n,
    chosen_ref,
    tokens_hbm,
    wq_hbm,
    wk_hbm,
    wv_hbm,
    wo_hbm,
    normed_ref,
    logs_ref,
    tok,
    wq,
    wkv,
    wo,
    cos_t,
    sin_t,
    pick,
    bias,
    keys,
    vals_t,
    sel_k,
    sel_v,
    got_k,
    got_v,
    hot_s,
    q_raw,
    v_blk,
    qaug,
    m_s,
    l_s,
    acc,
    att,
    send_p,
    recv_p,
    load_sem,
    tok_sem,
    pick_send,
    pick_recv,
    k_send,
    k_recv,
    v_send,
    v_recv,
    p_send,
    p_recv,
):
    me = lax.axis_index("kv")
    half = lax.axis_index("tp")
    other = 1 - half
    rows = tok.shape[0]
    mine = rows // 2
    blocks = rows // BLK
    groups = wq.shape[1] // (2 * HEAD_DIM)
    slot_keys = CAP * BLK
    lanes_all = groups * BLK

    own_rows = pl.ds(pl.multiple_of(half * mine, mine), mine)
    ld_tok = pltpu.make_async_copy(tokens_hbm.at[0], tok.at[own_rows], load_sem.at[0])
    ld_k = pltpu.make_async_copy(wk_hbm, wkv.at[:, 0:128], load_sem.at[1])
    ld_v = pltpu.make_async_copy(wv_hbm, wkv.at[:, 128:256], load_sem.at[2])
    ld_q = pltpu.make_async_copy(wq_hbm, wq, load_sem.at[3])
    ld_tok.start()
    ld_k.start()
    ld_v.start()
    ld_q.start()
    ld_o = []
    for h in range(2):
        for g in range(groups):
            source = (h * groups + g) * HEAD_DIM
            target = (g * 2 + h) * HEAD_DIM
            ld_o.append(
                pltpu.make_async_copy(
                    wo_hbm.at[source : source + HEAD_DIM],
                    wo.at[target : target + HEAD_DIM],
                    load_sem.at[4 + h * groups + g],
                )
            )
    for copy in ld_o:
        copy.start()

    barrier = pltpu.get_barrier_semaphore()
    pl.semaphore_signal(barrier, inc=1, device_id={"tp": other}, device_id_type=MESH)
    for d in range(1, n):
        pl.semaphore_signal(
            barrier, inc=1, device_id={"kv": lax.rem(me + d, n)}, device_id_type=MESH
        )

    npad = pick.shape[2]
    chosen = chosen_ref[0]
    block_ids = iota((blocks, npad), 1)
    picked = jnp.zeros((blocks, npad), F32)
    for k in range(chosen.shape[1]):
        picked = picked + (chosen[:, k : k + 1] == block_ids).astype(F32)
    pick[0] = picked

    pl.semaphore_wait(barrier, n)
    ld_tok.wait()
    tok_copy = pltpu.make_async_remote_copy(
        src_ref=tok.at[own_rows],
        dst_ref=tok.at[own_rows],
        send_sem=tok_sem.at[0],
        recv_sem=tok_sem.at[1],
        device_id={"tp": other},
        device_id_type=MESH,
    )
    tok_copy.start()

    def pick_copy(d, target):
        return pltpu.make_async_remote_copy(
            src_ref=pick.at[0],
            dst_ref=pick.at[d],
            send_sem=pick_send.at[d],
            recv_sem=pick_recv.at[d],
            device_id={"kv": target},
            device_id_type=MESH,
        )

    @pl.loop(1, me + 1)
    def _(d):
        pick_copy(d, me - d).start()

    lane = iota((1, 128), 1)
    inverse = jnp.exp((lane % 32).astype(F32) * (-math.log(THETA_BASE) / 32))
    sign = jnp.where(lane % 64 < 32, -1.0, 1.0)
    inner = iota((BLK, 128), 0).astype(F32) * inverse
    cos_in, sin_in = jnp.cos(inner), jnp.sin(inner)
    starts = (me * rows + iota((blocks, 128), 0) * BLK).astype(F32) * inverse
    cos_st, sin_st = jnp.cos(starts), jnp.sin(starts)
    for c in range(blocks):
        part = slice(c * BLK, (c + 1) * BLK)
        cs, sn = cos_st[c : c + 1], sin_st[c : c + 1]
        cos_t[part] = cs * cos_in - sn * sin_in
        sin_t[part] = (sn * cos_in + cs * sin_in) * sign

    slots = bias.shape[0]
    nslots = slots // slot_keys * CAP

    def slot_table(marks):
        needed = (jnp.max(marks, axis=0, keepdims=True) > 0).astype(F32)
        b_in, b_out = iota((npad, npad), 0), iota((npad, npad), 1)
        before = ((b_in // blocks == b_out // blocks) & (b_in < b_out)).astype(BF16)
        rank = mm(jnp.broadcast_to(needed, (8, npad)).astype(BF16), before)[0:1]
        rank = rank.astype(jnp.int32)
        place = iota((1, npad), 1) // blocks * CAP + rank
        fits = (needed > 0) & (rank < CAP)
        return jnp.where((iota((nslots, npad), 0) == place) & fits, 1.0, 0.0).astype(BF16)

    table = slot_table(picked)
    zero_rows = jnp.zeros((HEAD_DIM - blocks, npad), F32)
    twice = jnp.concatenate([picked, zero_rows, picked, zero_rows], axis=0).astype(BF16)
    reads = mm(table, twice, NT)
    lane_n = iota((nslots, 128), 1)
    reads = jnp.where(lane_n % 64 < blocks, (1.0 - reads) * NEGATIVE, 0.0).astype(BF16)
    spread = (iota((slots, nslots), 0) // BLK == iota((slots, nslots), 1)).astype(BF16)
    bias[...] = mm(spread, reads).astype(BF16)

    def rope(x, part):
        turned = jnp.where(
            iota(x.shape, 1) % 64 < 32, pltpu.roll(x, 96, 1), pltpu.roll(x, 32, 1)
        )
        return x * cos_t[part] + turned * sin_t[part]

    def selector(tab, d):
        first = (
            iota((slot_keys, nslots), 1) == me * CAP + iota((slot_keys, nslots), 0) // BLK
        ).astype(BF16)
        last = (iota((npad, rows), 0) == me * blocks + iota((npad, rows), 1) // BLK).astype(BF16)
        chain = mm(mm(first, tab).astype(BF16), last)
        same = iota((slot_keys, rows), 0) % BLK == iota((slot_keys, rows), 1) % BLK
        hot_s[d] = jnp.where(same, chain, 0.0).astype(BF16)

    selector(table, 0)

    own_part = pl.ds(pl.multiple_of(half * mine, mine), mine)
    far_part = pl.ds(pl.multiple_of(other * mine, mine), mine)

    def project_kv(part):
        out = mm(tok[part], wkv[...]).astype(BF16)
        keys[part] = rope(out[:, 0:128].astype(F32), part).astype(BF16)
        vals_t[:, part] = out[:, 128:256].astype(F32).T.astype(BF16)

    def project_q(part):
        q_raw[part] = mm(tok[part], wq[...]).astype(BF16)

    ld_k.wait()
    ld_v.wait()
    project_kv(own_part)
    ld_q.wait()
    project_q(own_part)

    @pl.loop(1, n - me)
    def _(d):
        pick_copy(d, me).wait_recv()
        selector(slot_table(pick[d]), d)

    tok_copy.wait_recv()
    project_kv(far_part)

    def select(d):
        sel_k[d] = mm(hot_s[d], keys[...]).astype(BF16)
        sel_v[d] = mm(vals_t[...], hot_s[d], NT).astype(BF16)

    def key_copy(d, target):
        return pltpu.make_async_remote_copy(
            src_ref=sel_k.at[d],
            dst_ref=got_k.at[d],
            send_sem=k_send.at[d],
            recv_sem=k_recv.at[d],
            device_id={"kv": target},
            device_id_type=MESH,
        )

    def value_copy(d, target):
        return pltpu.make_async_remote_copy(
            src_ref=sel_v.at[d],
            dst_ref=got_v.at[d],
            send_sem=v_send.at[d],
            recv_sem=v_recv.at[d],
            device_id={"kv": target},
            device_id_type=MESH,
        )

    @pl.loop(1, n - me)
    def _(d):
        select(d)
        key_copy(d, me + d).start()
        value_copy(d, me + d).start()

    project_q(far_part)
    select(0)
    for c in range(blocks):
        v_blk[c] = vals_t[:, c * BLK : (c + 1) * BLK]

    for c in range(blocks):
        part = slice(c * BLK, (c + 1) * BLK)
        q = q_raw[part].astype(F32)
        tiles = [
            rope(q[:, t * 128 : (t + 1) * 128], part) * HEAD_DIM**-0.5 for t in range(groups)
        ]
        low = iota((BLK, 128), 1) < 64
        hot = (iota((BLK, 128), 1) % 64 == c).astype(F32)
        for g in range(groups):
            a, b = tiles[g // 2], tiles[groups // 2 + g // 2]
            if g % 2 == 0:
                both = jnp.where(low, a, pltpu.roll(b, 64, 1))
            else:
                both = jnp.where(low, pltpu.roll(a, 64, 1), b)
            place = slice(g * BLK, (g + 1) * BLK)
            qaug[c, 0, place] = jnp.where(low, both, hot).astype(BF16)
            qaug[c, 1, place] = jnp.where(low, hot, both).astype(BF16)

    def widened(k, extra, h):
        low = iota(k.shape, 1) < 64
        return jnp.where(low, k, extra) if h == 0 else jnp.where(low, extra, k)

    group = 2 if blocks % 2 == 0 else 1

    def tiles_of(i):
        return [(i * group + u, h) for u in range(group) for h in range(2)]

    def head_of(h):
        return slice(h * HEAD_DIM, (h + 1) * HEAD_DIM)

    own_bias = bias[pl.ds(pl.multiple_of(me * slot_keys, slot_keys), slot_keys)]
    k_slots = [widened(sel_k[0], own_bias, h) for h in range(2)]
    ok = iota((BLK, lanes_all), 0) <= iota((BLK, lanes_all), 1) % BLK

    @pl.loop(0, blocks // group)
    def _(i):
        done = []
        for c, h in tiles_of(i):
            q = qaug[c, h]
            k_own = keys[pl.ds(pl.multiple_of(c * BLK, BLK), BLK)]
            s = mm(k_slots[h], q, NT)
            s_own = mm(widened(k_own, jnp.zeros_like(k_own), h), q, NT)
            s_own = jnp.where(ok, s_own, NEGATIVE)
            m = jnp.maximum(
                jnp.max(s, axis=0, keepdims=True), jnp.max(s_own, axis=0, keepdims=True)
            )
            p = jnp.exp(s - m)
            p_own = jnp.exp(s_own - m)
            l = jnp.sum(p, axis=0, keepdims=True) + jnp.sum(p_own, axis=0, keepdims=True)
            o = mm(sel_v[0, head_of(h)], p.astype(BF16))
            o = o + mm(v_blk[c, head_of(h)], p_own.astype(BF16))
            done.append((m, l, o))
        for (c, h), (m, l, o) in zip(tiles_of(i), done):
            m_s[c, h] = m
            l_s[c, h] = l
            acc[c, h] = o

    @pl.loop(1, me + 1)
    def _(d):
        key_copy(d, me).wait_recv()
        value_copy(d, me).wait_recv()
        owner = me - d
        extra = bias[pl.ds(pl.multiple_of(owner * slot_keys, slot_keys), slot_keys)]
        ks = [widened(got_k[d], extra, h) for h in range(2)]

        @pl.loop(0, blocks // group)
        def _(i):
            done = []
            held = [(m_s[c, h], l_s[c, h], acc[c, h]) for c, h in tiles_of(i)]
            for (c, h), (m_old, l_old, o_old) in zip(tiles_of(i), held):
                s = mm(ks[h], qaug[c, h], NT)
                m = jnp.maximum(m_old, jnp.max(s, axis=0, keepdims=True))
                shrink = jnp.exp(m_old - m)
                p = jnp.exp(s - m)
                l = l_old * shrink + jnp.sum(p, axis=0, keepdims=True)
                o = o_old * shrink + mm(got_v[d, head_of(h)], p.astype(BF16))
                done.append((m, l, o))
            for (c, h), (m, l, o) in zip(tiles_of(i), done):
                m_s[c, h] = m
                l_s[c, h] = l
                acc[c, h] = o

    for c in range(blocks):
        part = slice(c * BLK, (c + 1) * BLK)
        sums = [l_s[c, h] for h in range(2)]
        both = jnp.concatenate([acc[c, h] / sums[h] for h in range(2)], axis=0).T
        for g in range(groups):
            att[part, g * 128 : (g + 1) * 128] = both[g * BLK : (g + 1) * BLK].astype(BF16)
        logs = [m_s[c, h] + jnp.log(sums[h]) for h in range(2)]
        stacked = jnp.concatenate(
            [logs[h][:, g * BLK : (g + 1) * BLK] for h in range(2) for g in range(groups)],
            axis=0,
        )
        logs_ref[0, :, part] = stacked

    for copy in ld_o:
        copy.wait()
    pieces = send_p.shape[0]
    step = mine // pieces

    def sum_copy(i):
        return pltpu.make_async_remote_copy(
            src_ref=send_p.at[i],
            dst_ref=recv_p.at[i],
            send_sem=p_send.at[i],
            recv_sem=p_recv.at[i],
            device_id={"tp": other},
            device_id_type=MESH,
        )

    for i in range(pieces):
        part = pl.ds(pl.multiple_of(other * mine + i * step, step), step)
        send_p[i] = mm(att[part], wo[...])
        sum_copy(i).start()
    for i in range(pieces):
        part = pl.ds(pl.multiple_of(half * mine + i * step, step), step)
        own = mm(att[part], wo[...])
        sum_copy(i).wait_recv()
        total = own + recv_p[i]
        scale = lax.rsqrt(jnp.mean(total * total, axis=-1, keepdims=True) + EPSILON)
        normed_ref[0, i * step : (i + 1) * step] = (total * scale).astype(BF16)

    tok_copy.wait_send()
    for i in range(pieces):
        sum_copy(i).wait_send()

    @pl.loop(1, me + 1)
    def _(d):
        pick_copy(d, me).wait_send()

    @pl.loop(1, n - me)
    def _(d):
        key_copy(d, me).wait_send()
        value_copy(d, me).wait_send()


def shards(tokens, w_query, w_key, w_value, w_out, chosen):
    n = lax.axis_size("kv")
    mine, width = tokens.shape[1], tokens.shape[2]
    rows = 2 * mine
    blocks = rows // BLK
    heads = w_query.shape[1] // HEAD_DIM
    groups = heads // 2
    npad = -(-n * blocks // 128) * 128
    slot_keys = CAP * BLK
    lanes_all = groups * BLK
    pieces = 2
    dma = pltpu.SemaphoreType.DMA
    vmem = pl.BlockSpec(memory_space=pltpu.VMEM)
    hbm = pl.BlockSpec(memory_space=pl.ANY)
    normed, logs = pl.pallas_call(
        functools.partial(kernel, n),
        out_shape=(
            jax.ShapeDtypeStruct((1, mine, width), BF16),
            jax.ShapeDtypeStruct((1, heads, rows), F32),
        ),
        in_specs=[vmem, hbm, hbm, hbm, hbm, hbm],
        out_specs=(vmem, vmem),
        scratch_shapes=[
            pltpu.VMEM((rows, width), BF16),
            pltpu.VMEM(w_query.shape, BF16),
            pltpu.VMEM((width, 256), BF16),
            pltpu.VMEM(w_out.shape, BF16),
            pltpu.VMEM((rows, 128), F32),
            pltpu.VMEM((rows, 128), F32),
            pltpu.VMEM((n, blocks, npad), F32),
            pltpu.VMEM((n * slot_keys, 128), BF16),
            pltpu.VMEM((rows, 128), BF16),
            pltpu.VMEM((128, rows), BF16),
            pltpu.VMEM((n, slot_keys, 128), BF16),
            pltpu.VMEM((n, 128, slot_keys), BF16),
            pltpu.VMEM((n, slot_keys, 128), BF16),
            pltpu.VMEM((n, 128, slot_keys), BF16),
            pltpu.VMEM((n, slot_keys, rows), BF16),
            pltpu.VMEM((rows, w_query.shape[1]), BF16),
            pltpu.VMEM((blocks, 128, BLK), BF16),
            pltpu.VMEM((blocks, 2, lanes_all, 128), BF16),
            pltpu.VMEM((blocks, 2, 1, lanes_all), F32),
            pltpu.VMEM((blocks, 2, 1, lanes_all), F32),
            pltpu.VMEM((blocks, 2, HEAD_DIM, lanes_all), F32),
            pltpu.VMEM((rows, heads * HEAD_DIM), BF16),
            pltpu.VMEM((pieces, mine // pieces, width), F32),
            pltpu.VMEM((pieces, mine // pieces, width), F32),
            dma((4 + heads,)),
            dma((2,)),
            dma((n,)),
            dma((n,)),
            dma((n,)),
            dma((n,)),
            dma((n,)),
            dma((n,)),
            dma((pieces,)),
            dma((pieces,)),
        ],
        compiler_params=pltpu.CompilerParams(
            collective_id=0, has_side_effects=True, vmem_limit_bytes=67043328
        ),
    )(chosen, tokens, w_query, w_key, w_value, w_out)
    return normed, jnp.swapaxes(logs, 1, 2)


def solution(mesh):
    placed = (
        P("dp", ("kv", "tp"), None),
        P(None, "tp"),
        P(None, "tp"),
        P(None, "tp"),
        P("tp", None),
        P("dp", "kv", None),
    )
    return jax.shard_map(
        shards,
        mesh=mesh,
        in_specs=placed,
        out_specs=(P("dp", ("kv", "tp"), None), P("dp", "kv", "tp")),
        check_vma=False,
    )
```

```python
import functools
import math

import jax
import jax.numpy as jnp
from jax import lax
from jax.experimental import pallas as pl
from jax.experimental.pallas import tpu as pltpu
from jax.sharding import PartitionSpec as P

HEAD_DIM = 64
BLK = 64
CAP = 4
THETA_BASE = 10000.0
NEGATIVE = -1e30
EPSILON = 1e-06
MESH = pl.DeviceIdType.MESH
F32 = jnp.float32
BF16 = jnp.bfloat16
NT = (((1,), (1,)), ((), ()))
NN = (((1,), (0,)), ((), ()))


def mm(a, b, dims=NN):
    return lax.dot_general(a, b, dims, preferred_element_type=F32)


def iota(shape, dim):
    return lax.broadcasted_iota(jnp.int32, shape, dim)


def kernel(
    n,
    chosen_ref,
    tokens_hbm,
    wq_hbm,
    wk_hbm,
    wv_hbm,
    wo_hbm,
    normed_ref,
    logs_ref,
    tok,
    wq,
    wkv,
    wo,
    cos_t,
    sin_t,
    pick,
    bias,
    keys,
    vals_t,
    sel_k,
    sel_v,
    got_k,
    got_v,
    hot_s,
    q_raw,
    v_blk,
    qaug,
    m_s,
    l_s,
    acc,
    att,
    send_p,
    recv_p,
    load_sem,
    tok_sem,
    pick_send,
    pick_recv,
    k_send,
    k_recv,
    v_send,
    v_recv,
    p_send,
    p_recv,
):
    me = lax.axis_index("kv")
    half = lax.axis_index("tp")
    other = 1 - half
    rows = tok.shape[0]
    mine = rows // 2
    blocks = rows // BLK
    groups = wq.shape[1] // (2 * HEAD_DIM)
    slot_keys = CAP * BLK
    lanes_all = groups * BLK

    own_rows = pl.ds(pl.multiple_of(half * mine, mine), mine)
    ld_tok = pltpu.make_async_copy(tokens_hbm.at[0], tok.at[own_rows], load_sem.at[0])
    ld_k = pltpu.make_async_copy(wk_hbm, wkv.at[:, 0:128], load_sem.at[1])
    ld_v = pltpu.make_async_copy(wv_hbm, wkv.at[:, 128:256], load_sem.at[2])
    ld_q = pltpu.make_async_copy(wq_hbm, wq, load_sem.at[3])
    ld_tok.start()
    ld_k.start()
    ld_v.start()
    ld_q.start()
    ld_o = []
    for h in range(2):
        for g in range(groups):
            source = (h * groups + g) * HEAD_DIM
            target = (g * 2 + h) * HEAD_DIM
            ld_o.append(
                pltpu.make_async_copy(
                    wo_hbm.at[source : source + HEAD_DIM],
                    wo.at[target : target + HEAD_DIM],
                    load_sem.at[4 + h * groups + g],
                )
            )
    for copy in ld_o:
        copy.start()

    barrier = pltpu.get_barrier_semaphore()
    pl.semaphore_signal(barrier, inc=1, device_id={"tp": other}, device_id_type=MESH)
    for d in range(1, n):
        pl.semaphore_signal(
            barrier, inc=1, device_id={"kv": lax.rem(me + d, n)}, device_id_type=MESH
        )

    npad = pick.shape[2]
    chosen = chosen_ref[0]
    block_ids = iota((blocks, npad), 1)
    picked = jnp.zeros((blocks, npad), F32)
    for k in range(chosen.shape[1]):
        picked = picked + (chosen[:, k : k + 1] == block_ids).astype(F32)
    pick[0] = picked

    pl.semaphore_wait(barrier, n)
    ld_tok.wait()
    tok_copy = pltpu.make_async_remote_copy(
        src_ref=tok.at[own_rows],
        dst_ref=tok.at[own_rows],
        send_sem=tok_sem.at[0],
        recv_sem=tok_sem.at[1],
        device_id={"tp": other},
        device_id_type=MESH,
    )
    tok_copy.start()

    def pick_copy(d, target):
        return pltpu.make_async_remote_copy(
            src_ref=pick.at[0],
            dst_ref=pick.at[d],
            send_sem=pick_send.at[d],
            recv_sem=pick_recv.at[d],
            device_id={"kv": target},
            device_id_type=MESH,
        )

    @pl.loop(1, me + 1)
    def _(d):
        pick_copy(d, me - d).start()

    lane = iota((1, 128), 1)
    inverse = jnp.exp((lane % 32).astype(F32) * (-math.log(THETA_BASE) / 32))
    sign = jnp.where(lane % 64 < 32, -1.0, 1.0)
    inner = iota((BLK, 128), 0).astype(F32) * inverse
    cos_in, sin_in = jnp.cos(inner), jnp.sin(inner)
    starts = (me * rows + iota((blocks, 128), 0) * BLK).astype(F32) * inverse
    cos_st, sin_st = jnp.cos(starts), jnp.sin(starts)
    for c in range(blocks):
        part = slice(c * BLK, (c + 1) * BLK)
        cs, sn = cos_st[c : c + 1], sin_st[c : c + 1]
        cos_t[part] = cs * cos_in - sn * sin_in
        sin_t[part] = (sn * cos_in + cs * sin_in) * sign

    slots = bias.shape[0]
    nslots = slots // slot_keys * CAP

    def slot_table(marks):
        needed = (jnp.max(marks, axis=0, keepdims=True) > 0).astype(F32)
        b_in, b_out = iota((npad, npad), 0), iota((npad, npad), 1)
        before = ((b_in // blocks == b_out // blocks) & (b_in < b_out)).astype(BF16)
        rank = mm(jnp.broadcast_to(needed, (8, npad)).astype(BF16), before)[0:1]
        rank = rank.astype(jnp.int32)
        place = iota((1, npad), 1) // blocks * CAP + rank
        fits = (needed > 0) & (rank < CAP)
        return jnp.where((iota((nslots, npad), 0) == place) & fits, 1.0, 0.0).astype(BF16)

    table = slot_table(picked)
    zero_rows = jnp.zeros((HEAD_DIM - blocks, npad), F32)
    twice = jnp.concatenate([picked, zero_rows, picked, zero_rows], axis=0).astype(BF16)
    reads = mm(table, twice, NT)
    lane_n = iota((nslots, 128), 1)
    reads = jnp.where(lane_n % 64 < blocks, (1.0 - reads) * NEGATIVE, 0.0).astype(BF16)
    spread = (iota((slots, nslots), 0) // BLK == iota((slots, nslots), 1)).astype(BF16)
    bias[...] = mm(spread, reads).astype(BF16)

    def rope(x, part):
        turned = jnp.where(
            iota(x.shape, 1) % 64 < 32, pltpu.roll(x, 96, 1), pltpu.roll(x, 32, 1)
        )
        return x * cos_t[part] + turned * sin_t[part]

    def selector(tab, d):
        first = (
            iota((slot_keys, nslots), 1) == me * CAP + iota((slot_keys, nslots), 0) // BLK
        ).astype(BF16)
        last = (iota((npad, rows), 0) == me * blocks + iota((npad, rows), 1) // BLK).astype(BF16)
        chain = mm(mm(first, tab).astype(BF16), last)
        same = iota((slot_keys, rows), 0) % BLK == iota((slot_keys, rows), 1) % BLK
        hot_s[d] = jnp.where(same, chain, 0.0).astype(BF16)

    selector(table, 0)

    own_part = pl.ds(pl.multiple_of(half * mine, mine), mine)
    far_part = pl.ds(pl.multiple_of(other * mine, mine), mine)

    def project_kv(part):
        out = mm(tok[part], wkv[...]).astype(BF16)
        keys[part] = rope(out[:, 0:128].astype(F32), part).astype(BF16)
        vals_t[:, part] = out[:, 128:256].astype(F32).T.astype(BF16)

    ld_k.wait()
    ld_v.wait()
    project_kv(own_part)

    @pl.loop(1, n - me)
    def _(d):
        pick_copy(d, me).wait_recv()
        selector(slot_table(pick[d]), d)

    tok_copy.wait_recv()
    project_kv(far_part)

    def select(d):
        sel_k[d] = mm(hot_s[d], keys[...]).astype(BF16)
        sel_v[d] = mm(vals_t[...], hot_s[d], NT).astype(BF16)

    def key_copy(d, target):
        return pltpu.make_async_remote_copy(
            src_ref=sel_k.at[d],
            dst_ref=got_k.at[d],
            send_sem=k_send.at[d],
            recv_sem=k_recv.at[d],
            device_id={"kv": target},
            device_id_type=MESH,
        )

    def value_copy(d, target):
        return pltpu.make_async_remote_copy(
            src_ref=sel_v.at[d],
            dst_ref=got_v.at[d],
            send_sem=v_send.at[d],
            recv_sem=v_recv.at[d],
            device_id={"kv": target},
            device_id_type=MESH,
        )

    @pl.loop(1, n - me)
    def _(e):
        d = n - me - e
        select(d)
        key_copy(d, me + d).start()
        value_copy(d, me + d).start()

    ld_q.wait()
    q_raw[...] = mm(tok[...], wq[...]).astype(BF16)
    select(0)
    for c in range(blocks):
        v_blk[c] = vals_t[:, c * BLK : (c + 1) * BLK]

    for c in range(blocks):
        part = slice(c * BLK, (c + 1) * BLK)
        q = q_raw[part].astype(F32)
        tiles = [
            rope(q[:, t * 128 : (t + 1) * 128], part) * HEAD_DIM**-0.5 for t in range(groups)
        ]
        low = iota((BLK, 128), 1) < 64
        hot = (iota((BLK, 128), 1) % 64 == c).astype(F32)
        for g in range(groups):
            a, b = tiles[g // 2], tiles[groups // 2 + g // 2]
            if g % 2 == 0:
                both = jnp.where(low, a, pltpu.roll(b, 64, 1))
            else:
                both = jnp.where(low, pltpu.roll(a, 64, 1), b)
            place = slice(g * BLK, (g + 1) * BLK)
            qaug[c, 0, place] = jnp.where(low, both, hot).astype(BF16)
            qaug[c, 1, place] = jnp.where(low, hot, both).astype(BF16)

    def widened(k, extra, h):
        low = iota(k.shape, 1) < 64
        return jnp.where(low, k, extra) if h == 0 else jnp.where(low, extra, k)

    group = 2 if blocks % 2 == 0 else 1

    def tiles_of(i):
        return [(i * group + u, h) for u in range(group) for h in range(2)]

    def head_of(h):
        return slice(h * HEAD_DIM, (h + 1) * HEAD_DIM)

    own_bias = bias[pl.ds(pl.multiple_of(me * slot_keys, slot_keys), slot_keys)]
    k_slots = [widened(sel_k[0], own_bias, h) for h in range(2)]
    ok = iota((BLK, lanes_all), 0) <= iota((BLK, lanes_all), 1) % BLK

    @pl.loop(0, blocks // group)
    def _(i):
        done = []
        for c, h in tiles_of(i):
            q = qaug[c, h]
            k_own = keys[pl.ds(pl.multiple_of(c * BLK, BLK), BLK)]
            s = mm(k_slots[h], q, NT)
            s_own = mm(widened(k_own, jnp.zeros_like(k_own), h), q, NT)
            s_own = jnp.where(ok, s_own, NEGATIVE)
            m = jnp.maximum(
                jnp.max(s, axis=0, keepdims=True), jnp.max(s_own, axis=0, keepdims=True)
            )
            p = jnp.exp(s - m)
            p_own = jnp.exp(s_own - m)
            l = jnp.sum(p, axis=0, keepdims=True) + jnp.sum(p_own, axis=0, keepdims=True)
            o = mm(sel_v[0, head_of(h)], p.astype(BF16))
            o = o + mm(v_blk[c, head_of(h)], p_own.astype(BF16))
            done.append((m, l, o))
        for (c, h), (m, l, o) in zip(tiles_of(i), done):
            m_s[c, h] = m
            l_s[c, h] = l
            acc[c, h] = o

    @pl.loop(1, me + 1)
    def _(d):
        key_copy(d, me).wait_recv()
        value_copy(d, me).wait_recv()
        owner = me - d
        extra = bias[pl.ds(pl.multiple_of(owner * slot_keys, slot_keys), slot_keys)]
        ks = [widened(got_k[d], extra, h) for h in range(2)]

        @pl.loop(0, blocks // group)
        def _(i):
            done = []
            held = [(m_s[c, h], l_s[c, h], acc[c, h]) for c, h in tiles_of(i)]
            for (c, h), (m_old, l_old, o_old) in zip(tiles_of(i), held):
                s = mm(ks[h], qaug[c, h], NT)
                m = jnp.maximum(m_old, jnp.max(s, axis=0, keepdims=True))
                shrink = jnp.exp(m_old - m)
                p = jnp.exp(s - m)
                l = l_old * shrink + jnp.sum(p, axis=0, keepdims=True)
                o = o_old * shrink + mm(got_v[d, head_of(h)], p.astype(BF16))
                done.append((m, l, o))
            for (c, h), (m, l, o) in zip(tiles_of(i), done):
                m_s[c, h] = m
                l_s[c, h] = l
                acc[c, h] = o

    for c in range(blocks):
        part = slice(c * BLK, (c + 1) * BLK)
        sums = [l_s[c, h] for h in range(2)]
        both = jnp.concatenate([acc[c, h] / sums[h] for h in range(2)], axis=0).T
        for g in range(groups):
            att[part, g * 128 : (g + 1) * 128] = both[g * BLK : (g + 1) * BLK].astype(BF16)
        logs = [m_s[c, h] + jnp.log(sums[h]) for h in range(2)]
        stacked = jnp.concatenate(
            [logs[h][:, g * BLK : (g + 1) * BLK] for h in range(2) for g in range(groups)],
            axis=0,
        )
        logs_ref[0, :, part] = stacked

    for copy in ld_o:
        copy.wait()
    pieces = send_p.shape[0]
    step = mine // pieces

    def sum_copy(i):
        return pltpu.make_async_remote_copy(
            src_ref=send_p.at[i],
            dst_ref=recv_p.at[i],
            send_sem=p_send.at[i],
            recv_sem=p_recv.at[i],
            device_id={"tp": other},
            device_id_type=MESH,
        )

    for i in range(pieces):
        part = pl.ds(pl.multiple_of(other * mine + i * step, step), step)
        send_p[i] = mm(att[part], wo[...])
        sum_copy(i).start()
    for i in range(pieces):
        part = pl.ds(pl.multiple_of(half * mine + i * step, step), step)
        own = mm(att[part], wo[...])
        sum_copy(i).wait_recv()
        total = own + recv_p[i]
        scale = lax.rsqrt(jnp.mean(total * total, axis=-1, keepdims=True) + EPSILON)
        normed_ref[0, i * step : (i + 1) * step] = (total * scale).astype(BF16)

    tok_copy.wait_send()
    for i in range(pieces):
        sum_copy(i).wait_send()

    @pl.loop(1, me + 1)
    def _(d):
        pick_copy(d, me).wait_send()

    @pl.loop(1, n - me)
    def _(d):
        key_copy(d, me).wait_send()
        value_copy(d, me).wait_send()


def shards(tokens, w_query, w_key, w_value, w_out, chosen):
    n = lax.axis_size("kv")
    mine, width = tokens.shape[1], tokens.shape[2]
    rows = 2 * mine
    blocks = rows // BLK
    heads = w_query.shape[1] // HEAD_DIM
    groups = heads // 2
    npad = -(-n * blocks // 128) * 128
    slot_keys = CAP * BLK
    lanes_all = groups * BLK
    pieces = 2
    dma = pltpu.SemaphoreType.DMA
    vmem = pl.BlockSpec(memory_space=pltpu.VMEM)
    hbm = pl.BlockSpec(memory_space=pl.ANY)
    normed, logs = pl.pallas_call(
        functools.partial(kernel, n),
        out_shape=(
            jax.ShapeDtypeStruct((1, mine, width), BF16),
            jax.ShapeDtypeStruct((1, heads, rows), F32),
        ),
        in_specs=[vmem, hbm, hbm, hbm, hbm, hbm],
        out_specs=(vmem, vmem),
        scratch_shapes=[
            pltpu.VMEM((rows, width), BF16),
            pltpu.VMEM(w_query.shape, BF16),
            pltpu.VMEM((width, 256), BF16),
            pltpu.VMEM(w_out.shape, BF16),
            pltpu.VMEM((rows, 128), F32),
            pltpu.VMEM((rows, 128), F32),
            pltpu.VMEM((n, blocks, npad), F32),
            pltpu.VMEM((n * slot_keys, 128), BF16),
            pltpu.VMEM((rows, 128), BF16),
            pltpu.VMEM((128, rows), BF16),
            pltpu.VMEM((n, slot_keys, 128), BF16),
            pltpu.VMEM((n, 128, slot_keys), BF16),
            pltpu.VMEM((n, slot_keys, 128), BF16),
            pltpu.VMEM((n, 128, slot_keys), BF16),
            pltpu.VMEM((n, slot_keys, rows), BF16),
            pltpu.VMEM((rows, w_query.shape[1]), BF16),
            pltpu.VMEM((blocks, 128, BLK), BF16),
            pltpu.VMEM((blocks, 2, lanes_all, 128), BF16),
            pltpu.VMEM((blocks, 2, 1, lanes_all), F32),
            pltpu.VMEM((blocks, 2, 1, lanes_all), F32),
            pltpu.VMEM((blocks, 2, HEAD_DIM, lanes_all), F32),
            pltpu.VMEM((rows, heads * HEAD_DIM), BF16),
            pltpu.VMEM((pieces, mine // pieces, width), F32),
            pltpu.VMEM((pieces, mine // pieces, width), F32),
            dma((4 + heads,)),
            dma((2,)),
            dma((n,)),
            dma((n,)),
            dma((n,)),
            dma((n,)),
            dma((n,)),
            dma((n,)),
            dma((pieces,)),
            dma((pieces,)),
        ],
        compiler_params=pltpu.CompilerParams(
            collective_id=0, has_side_effects=True, vmem_limit_bytes=67043328
        ),
    )(chosen, tokens, w_query, w_key, w_value, w_out)
    return normed, jnp.swapaxes(logs, 1, 2)


def solution(mesh):
    placed = (
        P("dp", ("kv", "tp"), None),
        P(None, "tp"),
        P(None, "tp"),
        P(None, "tp"),
        P("tp", None),
        P("dp", "kv", None),
    )
    return jax.shard_map(
        shards,
        mesh=mesh,
        in_specs=placed,
        out_specs=(P("dp", ("kv", "tp"), None), P("dp", "kv", "tp")),
        check_vma=False,
    )
```
